512 devices in a mesh: rep: 2 (over z_hi), fs: 32 (over z_lo, y), tp: 8 (over x, core).
Axes of the slice: x: 4, y: 4, z: 16 (z_hi: 2, z_lo: 8; z = z_hi * 8 + z_lo), core: 2. Of those that a mesh axis runs over, the one named last changes fastest.
Arguments:
- tokens: bfloat16 [49152, 2048], P(('rep', 'fs', 'tp')), may hold values from -6 to 6
- norm_gain: float32 [2048], replicated, may hold values from 0.1 to 1.9
- gate_weight: float32 [2048, 5632], P('fs', 'tp'), may hold values from -0.125 to 0.125
- up_weight: float32 [2048, 5632], P('fs', 'tp'), may hold values from -0.125 to 0.125
- gate_scale: float32 [5632], P('tp'), may hold values from 0.3 to 3
- up_scale: float32 [5632], P('tp'), may hold values from 0.3 to 3
- down_weight: float32 [5632, 2048], P('tp', 'fs'), may hold values from -0.078125 to 0.078125
- down_scale: float32 [2048], replicated, may hold values from 0.3 to 3
Outputs:
- mixed: bfloat16 [49152, 2048], P(('rep', 'fs', 'tp'))
The draws below stay inside these ranges and needn't reach their ends.
All inputs are finite; a program needn't handle non-finite values.
Results may differ from the reference program's by a relative error of at most 0.014.
Values may be sent and summed in bfloat16 or wider, within the bound.
A program may use at most 64 MiB of HBM per device.

```python
import math
import jax
import jax.numpy as jnp
from jax import lax

D = 2048
FF = 5632
TOKENS = 49152
N_TP = 8


def level_of(own_key, dims, pieces, smallest, largest):
    def one(axis_at, blocks):
        steps = jax.random.uniform(jax.random.fold_in(jax.random.fold_in(own_key, 6), axis_at), (blocks,), jnp.float32, smallest / len(pieces), largest / len(pieces))
        return jnp.repeat(jnp.exp(steps), dims[axis_at] // blocks).reshape((-1,) + (1,) * (len(dims) - axis_at - 1))

    level = one(*pieces[0])
    for cut in pieces[1:]:
        level = level * one(*cut)
    return level


def gaussian(key, extent, scale, bound, cuts=(), held_as=jnp.bfloat16):
    drawn = scale * jax.random.normal(key, extent, jnp.float32)
    if cuts:
        drawn = drawn * level_of(key, extent, cuts, -0.22, 0.18)
    return jnp.clip(drawn, -bound, bound).astype(held_as)


def setup_inputs(seed: int = 0) -> dict:
    splits = jax.random.split(jax.random.key(seed), 9)
    tokens = gaussian(splits[0], (TOKENS, D), 1.0, 6.0, ((0, 512),))
    norm_gain = jnp.clip(1.0 + 0.18 * jax.random.normal(splits[1], (D,), jnp.float32), 0.1, 1.9)
    gate_weight = gaussian(splits[2], (D, FF), D ** -0.5, 0.125, ((0, 32), (1, 8)), jnp.float32)
    up_weight = gaussian(splits[3], (D, FF), D ** -0.5, 0.125, ((0, 32), (1, 8)), jnp.float32)
    gate_scale = jnp.clip(jnp.exp(math.log(3.0) - 2.3025851 * jax.random.uniform(splits[4], (FF,), jnp.float32) ** level_of(splits[4], (FF,), ((0, 8),), -0.2, 0.2)), 0.3, 3.0)
    up_scale = jnp.clip(jnp.exp(math.log(3.0) - 2.3025851 * jax.random.uniform(splits[5], (FF,), jnp.float32) ** level_of(splits[5], (FF,), ((0, 8),), -0.2, 0.2)), 0.3, 3.0)
    down_weight = gaussian(splits[6], (FF, D), FF ** -0.5, 0.078125, ((0, 8), (1, 32)), jnp.float32)
    down_scale = jnp.clip(jnp.exp(jax.random.uniform(splits[7], (D,), jnp.float32, math.log(0.3), math.log(3.0))), 0.3, 3.0)
    return {"tokens": tokens, "norm_gain": norm_gain, "gate_weight": gate_weight, "up_weight": up_weight, "gate_scale": gate_scale, "up_scale": up_scale, "down_weight": down_weight, "down_scale": down_scale}


def reference(tokens, norm_gain, gate_weight, up_weight, gate_scale, up_scale, down_weight, down_scale):
    values = tokens.astype(jnp.float32)
    normed = (values * lax.rsqrt(lax.optimization_barrier(jnp.mean(values * values, axis=-1, keepdims=True)) + 1e-06) * norm_gain).astype(jnp.bfloat16)
    block_width = FF // N_TP
    gate_blocks = gate_weight.astype(jnp.bfloat16).reshape(D, N_TP, block_width).transpose(1, 0, 2)
    up_blocks = up_weight.astype(jnp.bfloat16).reshape(D, N_TP, block_width).transpose(1, 0, 2)
    down_blocks = down_weight.astype(jnp.bfloat16).reshape(N_TP, block_width, D)
    gate_scales = gate_scale.reshape(N_TP, block_width)
    up_scales = up_scale.reshape(N_TP, block_width)

    def one_block(running, blocks):
        gate_piece, up_piece, gate_factor, up_factor, down_piece = blocks
        gate_value = jnp.dot(normed, gate_piece, preferred_element_type=jnp.float32) * gate_factor
        up_value = jnp.dot(normed, up_piece, preferred_element_type=jnp.float32) * up_factor
        hidden = (jax.nn.silu(gate_value) * up_value).astype(jnp.bfloat16)
        partial_value = jnp.dot(hidden, down_piece, preferred_element_type=jnp.float32).astype(jnp.bfloat16)
        return (running + partial_value.astype(jnp.float32), None)
    summed, unused = lax.scan(one_block, jnp.zeros((tokens.shape[0], D), jnp.float32), (gate_blocks, up_blocks, gate_scales, up_scales, down_blocks))
    return (summed * down_scale).astype(jnp.bfloat16)
```

```python
import jax
import jax.numpy as jnp
from jax import lax
from jax.experimental import pallas as pl
from jax.experimental.pallas import tpu as pltpu
from jax.sharding import PartitionSpec as P

BF16 = jnp.bfloat16
F32 = jnp.float32
D = 2048
ROWS = 96
ALL_ROWS = 768
NZ, NY, NX = 8, 4, 4
WA, WB = 640, 768
DA, DK = 256, 768

ICI = 45e3
SIB = 500e3
LAT = 2.0
LAT_SIB = 1.0
ISSUE = 0.06
BACKLOG = 3.0
T_MM_A, T_MM_B, T_SILU, T_DN = 0.6, 0.7, 2.5, 0.7
T_RED1, T_RED2, T_FIN = 0.3, 0.2, 0.2


class Send:
    def __init__(self, link, src, dst, nbytes, deps, prio, after=0.0):
        self.link, self.src, self.dst, self.nbytes = link, src, dst, nbytes
        self.deps, self.prio, self.after = deps, prio, after
        self.idx = None


class Task:
    def __init__(self, kind, unit, deps, gives, dur, prio):
        self.kind, self.unit, self.deps, self.gives = kind, unit, deps, gives
        self.dur, self.prio = dur, prio


def weight_sends(name, first, width, p1, p2, after):
    sends = []
    nb = 64 * width * 2
    whole, lo, hi = (0, 64), (0, 32), (32, 32)

    def add(link, dz, dy, part, ddz, ddy, deps, prio):
        sends.append(
            Send(
                link,
                (name, dz % 8, dy % 4, part),
                (name, (dz + ddz) % 8, (dy + ddy) % 4, part),
                nb * part[1] // 64,
                deps,
                prio,
                after,
            )
        )

    def key(dz, dy, part):
        return (name, dz % 8, dy % 4, part)

    def avail(dz, dy):
        if (dz, dy) == (0, 0):
            return [("own", name)]
        halves = (dy == 2) if first == "y" else (dz == 4)
        if halves and (dz == 0 if first == "y" else dy == 0):
            return [key(dz, dy, lo), key(dz, dy, hi)]
        return [key(dz, dy, whole)]

    if first == "y":
        own = avail(0, 0)
        add("y+", 0, 0, whole, 0, -1, own, p1)
        add("y-", 0, 0, whole, 0, 1, own, p1)
        add("y+", 0, 3, lo, 0, -1, [key(0, 3, whole)], p1)
        add("y-", 0, 1, hi, 0, 1, [key(0, 1, whole)], p1)
        for dy in range(4):
            for dz in (0, 7, 6, 5):
                if dz != 5 or dy in (0, 1):
                    add("z+", dz, dy, whole, -1, 0, avail(dz, dy), p2)
            for dz in (0, 1, 2, 3):
                if dz != 3 or dy in (2, 3):
                    add("z-", dz, dy, whole, 1, 0, avail(dz, dy), p2)
    else:
        for dz in (0, 7, 6):
            add("z+", dz, 0, whole, -1, 0, avail(dz, 0), p1)
        add("z+", 5, 0, lo, -1, 0, avail(5, 0), p1)
        for dz in (0, 1, 2):
            add("z-", dz, 0, whole, 1, 0, avail(dz, 0), p1)
        add("z-", 3, 0, hi, 1, 0, avail(3, 0), p1)
        for dz in range(8):
            add("y+", dz, 0, whole, 0, -1, avail(dz, 0), p2)
            add("y-", dz, 0, whole, 0, 1, avail(dz, 0), p2)
            if dz in (0, 6, 2, 4):
                add("y+", dz, 3, whole, 0, -1, avail(dz, 3), p2 - 0.1)
            else:
                add("y-", dz, 1, whole, 0, 1, avail(dz, 1), p2 - 0.1)
    return sends


def unit_keys(name, first, dz):
    whole, lo, hi = (0, 64), (0, 32), (32, 32)
    keys = []
    for dy in range(4):
        if (dz, dy) == (0, 0):
            keys.append(("own", name))
        elif first == "y" and dz == 0 and dy == 2 or first == "z" and dy == 0 and dz == 4:
            keys += [(name, dz, dy, lo), (name, dz, dy, hi)]
        else:
            keys.append((name, dz, dy, whole))
    return keys


def build():
    sends, tasks = [], []
    tasks.append(Task("prep", 0, [], [("own", n) for n in ("A", "B", "DA", "DB")], 1.0, -2))
    tasks.append(Task("norm", 0, [], [("own", "X")], 1.0, -1))
    sends += weight_sends("B", "z", WB, 0, 2, 0.0)
    sends += weight_sends("A", "y", WA, 0, 2, 0.0)
    sends += weight_sends("DB", "z", DK - DA, 1, 3, 8.0)
    sends += weight_sends("DA", "y", DA, 1, 3, 8.0)

    xb = 48 * D * 2
    ox = [("own", "X")]
    sends.append(Send("s", ("X", 0, 0, 2), ("X", 1, 0, 2), 2 * xb, ox, 0))
    for h in (0, 1):
        sends.append(Send("x+", ("X", 0, 0, h), ("X", 0, 3, h), xb, ox, h))
        sends.append(Send("x-", ("X", 0, 0, 1 - h), ("X", 0, 1, 1 - h), xb, ox, h))
    sends.append(Send("x+", ("X", 0, 3, 0), ("X", 0, 2, 0), xb, [("X", 0, 3, 0)], 0))
    sends.append(Send("x-", ("X", 0, 1, 1), ("X", 0, 2, 1), xb, [("X", 0, 1, 1)], 0))
    xkeys = [("own", "X"), ("X", 1, 0, 2)]
    for dx in (1, 2, 3):
        for h in (0, 1):
            sends.append(Send("s", ("X", 0, dx, h), ("X", 1, dx, h), xb, [("X", 0, dx, h)], 0))
            xkeys += [("X", 0, dx, h), ("X", 1, dx, h)]

    done = []
    for u in range(8):
        for n, first, dur in (("A", "y", T_MM_A), ("B", "z", T_MM_B)):
            tasks.append(
                Task("mm" + n, u, xkeys + unit_keys(n, first, u), [("mm", n, u)], dur, 5)
            )
            done.append(("mm", n, u))
    tasks.append(Task("silu", 0, done, [("H",)], T_SILU, 5))
    for u in range(8):
        dk = [("H",)] + unit_keys("DA", "y", u) + unit_keys("DB", "z", u)
        tasks.append(Task("dn", u, dk, [("P", u)], T_DN, 5))
        sends.append(Send("s", ("S", u), ("S", u), 4 * 96 * 256 * 2, [("P", u)], 0))
        tasks.append(Task("red1", u, [("P", u), ("S", u)], [("T", u)], T_RED1, 4))
        sends.append(Send("x-", ("T", u, 0), ("R", u, 0), 48 * 512, [("T", u)], 0))
        sends.append(Send("x+", ("T", u, 1), ("R", u, 1), 48 * 512, [("T", u)], 0))
        tasks.append(
            Task("red2", u, [("T", u), ("R", u, 0), ("R", u, 1)], [("N", u)], T_RED2, 3)
        )
        sends.append(Send("x-", ("N", u, 0), ("F", u, 0), 96 * 512, [("N", u)], 0))
        sends.append(Send("x+", ("N", u, 1), ("F", u, 1), 96 * 512, [("N", u)], 0))
        tasks.append(Task("fin", u, [("N", u), ("F", u, 0), ("F", u, 1)], [("O", u)], T_FIN, 2))
    return sends, tasks


def schedule():
    sends, tasks = build()
    for i, s in enumerate(sends):
        s.idx = i
    known, free, order = {}, {}, []
    t, left = 0.0, list(sends) + list(tasks)
    while left:
        best, soonest = None, None
        for o in left:
            if any(k not in known for k in o.deps):
                continue
            at = max([known[k] for k in o.deps], default=0.0)
            if isinstance(o, Send):
                at = max(at, o.after, free.get(o.link, 0.0) - BACKLOG)
                rank = (0, o.prio, at)
            else:
                rank = (1, o.prio, at)
            if at <= t + 1e-9:
                if best is None or rank < best[0]:
                    best = (rank, o)
            elif soonest is None or at < soonest:
                soonest = at
        if best is None:
            t = soonest
            continue
        o = best[1]
        left.remove(o)
        order.append((t, o))
        if isinstance(o, Send):
            t += ISSUE
            rate, lat = (SIB, LAT_SIB) if o.link == "s" else (ICI, LAT)
            free[o.link] = max(free.get(o.link, 0.0), t) + o.nbytes / rate
            known[o.dst] = free[o.link] + lat
        else:
            t += o.dur
            for k in o.gives:
                known[k] = t
    return sends, order, t


SENDS, ORDER, END = schedule()


def nt(a, b):
    return lax.dot_general(a, b, (((1,), (1,)), ((), ())), preferred_element_type=F32)


def kernel(
    tok, gain, gw, uw, gsc, usc, dw, dsc, out,
    xbuf, wa, wb, dbuf, acca, accb, hid, pown, ssend, srecv, tsend, rrecv, nsend, frecv,
    send_sems, recv_sems,
):
    rep, fs, tp = lax.axis_index("rep"), lax.axis_index("fs"), lax.axis_index("tp")
    zlo, y = fs // NY, fs % NY
    zg = rep * NZ + zlo
    x, c = tp // 2, tp % 2

    def zn(step):
        to = (zg + step + 16) % 16
        return (to // NZ, (to % NZ) * NY + y, tp)

    def yn(step):
        return (rep, zlo * NY + (y + step + NY) % NY, tp)

    def xn(step):
        return (rep, fs, ((x + step + NX) % NX) * 2 + c)

    peer = {
        "z+": zn(1), "z-": zn(-1), "y+": yn(1), "y-": yn(-1),
        "x+": xn(1), "x-": xn(-1), "s": (rep, fs, x * 2 + 1 - c),
    }
    barrier = pltpu.get_barrier_semaphore()
    for p in peer.values():
        pl.semaphore_signal(barrier, inc=1, device_id=p, device_id_type=pl.DeviceIdType.MESH)

    yrow = [pl.multiple_of(((y + dy) % NY) * 64, 64) for dy in range(NY)]

    def place(key):
        name = key[0]
        if name in ("A", "B", "DA", "DB"):
            _, dz, dy, (at, n) = key
            rows = pl.ds(yrow[dy] + at, n)
            if name == "A":
                return wa.at[dz, rows, :]
            if name == "B":
                return wb.at[dz, rows, :]
            if name == "DA":
                return dbuf.at[dz, rows, pl.ds(0, DA)]
            return dbuf.at[dz, rows, pl.ds(DA, DK - DA)]
        if name == "X":
            _, s, dx, h = key
            base = (s * 4 + dx) * ROWS
            return xbuf.at[:, pl.ds(base, ROWS) if h == 2 else pl.ds(base + h * 48, 48), :]
        if name == "T":
            return tsend.at[key[1], key[2]]
        if name == "R":
            return rrecv.at[key[1], key[2]]
        if name == "N":
            return nsend.at[key[1], key[2]]
        return frecv.at[key[1], key[2]]

    def outgoing(s):
        if s.src[0] == "S":
            src, dst = ssend.at[s.src[1]], srecv.at[s.src[1]]
        else:
            src, dst = place(s.src), None
            if s.dst[0] in ("A", "B", "DA", "DB"):
                name, dz, _, _ = s.dst
                _, _, dy, (at, n) = s.src
                rows = pl.ds(yrow[dy] + at, n)
                if name == "A":
                    dst = wa.at[dz, rows, :]
                elif name == "B":
                    dst = wb.at[dz, rows, :]
                elif name == "DA":
                    dst = dbuf.at[dz, rows, pl.ds(0, DA)]
                else:
                    dst = dbuf.at[dz, rows, pl.ds(DA, DK - DA)]
            else:
                dst = place(s.dst)
        return pltpu.make_async_remote_copy(
            src_ref=src, dst_ref=dst, send_sem=send_sems.at[s.idx], recv_sem=recv_sems.at[s.idx],
            device_id=peer[s.link], device_id_type=pl.DeviceIdType.MESH,
        )

    by_dst = {s.dst: s for s in SENDS}
    waited = set()

    def arrive(key):
        if key in waited or key not in by_dst:
            return
        waited.add(key)
        s = by_dst[key]
        ref = srecv.at[key[1]] if key[0] == "S" else place(key)
        pltpu.make_async_remote_copy(
            src_ref=ref, dst_ref=ref, send_sem=send_sems.at[s.idx], recv_sem=recv_sems.at[s.idx],
            device_id=peer[s.link], device_id_type=pl.DeviceIdType.MESH,
        ).wait_recv()

    first = {"A": True, "B": True}

    def run(o):
        u = o.unit
        if o.kind == "prep":
            mine = pl.ds(yrow[0], 64)
            g, v = gw[...], uw[...]
            wa[0, mine, :] = g[:, :WA].astype(BF16)
            wb[0, mine, pl.ds(0, WA)] = v[:, :WA].astype(BF16)
            mixed = jnp.concatenate([g[:, WA:], v[:, WA:]], axis=1)
            wb[0, mine, pl.ds(WA, 128)] = mixed.astype(BF16)
            dt = dw[...].T
            dbuf[0, mine, pl.ds(0, WA)] = dt[:, :WA].astype(BF16)
            tail = jnp.concatenate([dt[:, WA:], jnp.zeros((64, 64), F32)], axis=1)
            dbuf[0, mine, pl.ds(WA, 128)] = tail.astype(BF16)
            pl.semaphore_wait(barrier, 7)
        elif o.kind == "norm":
            v = tok[...].astype(F32)
            r = lax.rsqrt(jnp.mean(v * v, axis=-1, keepdims=True) + 1e-06)
            n = (v * r * gain[...]).astype(BF16)
            for k in range(NZ):
                xbuf[(k - zlo + NZ) % NZ, pl.ds(0, ROWS), :] = n[:, k * 256 : (k + 1) * 256]
        elif o.kind in ("mmA", "mmB"):
            n = o.kind[2]
            w, acc = (wa, acca) if n == "A" else (wb, accb)
            start, first[n] = first[n], False

            @pl.loop(0, 3)
            def _(i):
                rows = pl.ds(pl.multiple_of(i * 256, 256), 256)
                part = jnp.dot(xbuf[u, rows, :], w[u], preferred_element_type=F32)
                acc[rows, :] = part if start else acc[rows, :] + part
        elif o.kind == "silu":
            gs, us = gsc[...], usc[...]
            mixed_scale = jnp.concatenate([gs[:, WA:], us[:, WA:]], axis=1)
            low = lax.broadcasted_iota(jnp.int32, (32, 128), 1) < 64

            @pl.loop(0, ALL_ROWS // 32)
            def _(i):
                rows = pl.ds(pl.multiple_of(i * 32, 32), 32)
                g = acca[rows, :] * gs[:, :WA]
                v = accb[rows, pl.ds(0, WA)] * us[:, :WA]
                hid[rows, pl.ds(0, WA)] = (g / (1.0 + jnp.exp(-g)) * v).astype(BF16)
                m = accb[rows, pl.ds(WA, 128)] * mixed_scale
                h = m / (1.0 + jnp.exp(-m)) * pltpu.roll(m, 64, 1)
                hid[rows, pl.ds(WA, 128)] = jnp.where(low, h, 0.0).astype(BF16)
        elif o.kind == "dn":
            ssend[u] = nt(hid[pl.ds(384, 384), :], dbuf[u]).astype(BF16)
            pown[u] = nt(hid[pl.ds(0, 384), :], dbuf[u])
        elif o.kind == "red1":
            q = pown[u] + srecv[u].astype(F32)
            pown[u] = q
            tsend[u, 0] = q[192:240].astype(BF16)
            tsend[u, 1] = q[240:288].astype(BF16)
        elif o.kind == "red2":
            r0, r1 = rrecv[u, 0].astype(F32), rrecv[u, 1].astype(F32)
            nsend[u, 0, pl.ds(0, 48), :] = (pown[u, pl.ds(288, 48), :] + r0).astype(BF16)
            nsend[u, 0, pl.ds(48, 48), :] = pown[u, pl.ds(336, 48), :].astype(BF16)
            nsend[u, 1, pl.ds(0, 48), :] = pown[u, pl.ds(96, 48), :].astype(BF16)
            nsend[u, 1, pl.ds(48, 48), :] = (pown[u, pl.ds(144, 48), :] + r1).astype(BF16)
        elif o.kind == "fin":
            total = pown[u, pl.ds(0, 96), :] + frecv[u, 0].astype(F32) + frecv[u, 1].astype(F32)
            cols = pl.ds(pl.multiple_of(((zlo + u) % NZ) * 256, 256), 256)
            out[:, cols] = (total * dsc[:, cols]).astype(BF16)

    for _, o in ORDER:
        for k in o.deps:
            arrive(k)
        if isinstance(o, Send):
            outgoing(o).start()
        else:
            run(o)
    for s in SENDS:
        outgoing(s).wait_send()


def on_device(
    tokens, norm_gain, gate_weight, up_weight, gate_scale, up_scale, down_weight, down_scale
):
    n = len(SENDS)
    vm = pl.BlockSpec(memory_space=pltpu.VMEM)
    return pl.pallas_call(
        kernel,
        out_shape=jax.ShapeDtypeStruct((ROWS, D), BF16),
        in_specs=[vm] * 8,
        out_specs=vm,
        scratch_shapes=[
            pltpu.VMEM((8, ALL_ROWS, 256), BF16),
            pltpu.VMEM((8, 256, WA), BF16),
            pltpu.VMEM((8, 256, WB), BF16),
            pltpu.VMEM((8, 256, DK), BF16),
            pltpu.VMEM((ALL_ROWS, WA), F32),
            pltpu.VMEM((ALL_ROWS, WB), F32),
            pltpu.VMEM((ALL_ROWS, DK), BF16),
            pltpu.VMEM((8, 384, 256), F32),
            pltpu.VMEM((8, 384, 256), BF16),
            pltpu.VMEM((8, 384, 256), BF16),
            pltpu.VMEM((8, 2, 48, 256), BF16),
            pltpu.VMEM((8, 2, 48, 256), BF16),
            pltpu.VMEM((8, 2, 96, 256), BF16),
            pltpu.VMEM((8, 2, 96, 256), BF16),
            pltpu.SemaphoreType.DMA((n,)),
            pltpu.SemaphoreType.DMA((n,)),
        ],
        compiler_params=pltpu.CompilerParams(
            collective_id=0, has_side_effects=True, vmem_limit_bytes=60 * 1024 * 1024
        ),
    )(
        tokens, norm_gain[None], gate_weight, up_weight, gate_scale[None], up_scale[None],
        down_weight, down_scale[None],
    )


def solution(mesh):
    placed = (
        P(("rep", "fs", "tp"), None),
        P(),
        P("fs", "tp"),
        P("fs", "tp"),
        P("tp"),
        P("tp"),
        P("tp", "fs"),
        P(),
    )
    return jax.shard_map(
        on_device,
        mesh=mesh,
        in_specs=placed,
        out_specs=P(("rep", "fs", "tp"), None),
        check_vma=False,
    )
```

```python
import jax
import jax.numpy as jnp
from jax import lax
from jax.experimental import pallas as pl
from jax.experimental.pallas import tpu as pltpu
from jax.sharding import PartitionSpec as P

BF16 = jnp.bfloat16
F32 = jnp.float32
D = 2048
ROWS = 96
ALL_ROWS = 768
NZ, NY, NX = 8, 4, 4
WA, WB = 640, 768
DK = 768
SLOTS = 6

ICI, SIB = 45e3, 500e3
LAT, LAT_SIB = 2.3, 1.0
ISSUE, BACKLOG = 0.06, 1.5
COST = {
    "prep": 0.4, "norm": 0.5, "mmA": 0.35, "mmB": 0.4, "silu": 1.7, "dn": 0.4,
    "red1": 0.15, "red2": 0.12, "fin": 0.12,
}


class Send:
    def __init__(self, link, src, dst, nbytes, deps, prio):
        self.link, self.src, self.dst, self.nbytes = link, src, dst, nbytes
        self.deps, self.prio = deps, prio
        self.slot = self.sem = None


class Task:
    def __init__(self, kind, unit, deps, gives, prio):
        self.kind, self.unit, self.deps, self.gives = kind, unit, deps, gives
        self.dur, self.prio = COST[kind], prio


def unit_keys(name, first, dz, dys=(0, 1, 2, 3)):
    keys = []
    for dy in dys:
        if (dz, dy) == (0, 0):
            keys.append(("own", name))
        elif (first == "y" and dz == 0 and dy == 2) or (first == "z" and dy == 0 and dz == 4):
            keys += [(name, dz, dy, "l"), (name, dz, dy, "h")]
        else:
            keys.append((name, dz, dy, "w"))
    return keys


def weight_sends(name, first, nbytes, p1, p2):
    sends = []

    def add(link, dz, dy, part, ddz, ddy, prio):
        deps = unit_keys(name, first, dz, (dy,))
        size = nbytes if part == "w" else nbytes // 2
        dst = (name, (dz + ddz) % NZ, (dy + ddy) % NY, part)
        sends.append(Send(link, (name, dz, dy, part), dst, size, deps, prio))

    if first == "y":
        add("y+", 0, 0, "w", 0, -1, p1)
        add("y-", 0, 0, "w", 0, 1, p1)
        add("y+", 0, 3, "l", 0, -1, p1)
        add("y-", 0, 1, "h", 0, 1, p1)
        for dy in range(4):
            for dz in (0, 7, 6, 5):
                if dz != 5 or dy in (0, 1):
                    add("z+", dz, dy, "w", -1, 0, p2)
            for dz in (0, 1, 2, 3):
                if dz != 3 or dy in (2, 3):
                    add("z-", dz, dy, "w", 1, 0, p2)
    else:
        for dz in (0, 7, 6, 5):
            add("z+", dz, 0, "l" if dz == 5 else "w", -1, 0, p1)
        for dz in (0, 1, 2, 3):
            add("z-", dz, 0, "h" if dz == 3 else "w", 1, 0, p1)
        for dz in range(NZ):
            add("y+", dz, 0, "w", 0, -1, p2)
            add("y-", dz, 0, "w", 0, 1, p2)
            if dz in (0, 6, 2, 4):
                add("y+", dz, 3, "w", 0, -1, p2 - 0.1)
            else:
                add("y-", dz, 1, "w", 0, 1, p2 - 0.1)
    return sends


def build():
    sends, tasks = [], []
    tasks.append(Task("prep", 0, [], [("own", n) for n in ("A", "B", "DA", "DB")], -2))
    tasks.append(Task("norm", 0, [], [("own", "X")], -1))
    sends += weight_sends("B", "z", 64 * WB * 2, 0, 2)
    sends += weight_sends("A", "y", 64 * WA * 2, 0, 2)
    sends += weight_sends("DB", "z", 224 * 256, 2.5, 3)
    sends += weight_sends("DA", "y", 128 * 256, 2.5, 3)

    xb = 48 * D * 2
    ox = [("own", "X")]
    sends.append(Send("s", ("X", 0, 0, 2), ("X", 1, 0, 2), 2 * xb, ox, 0))
    for h in (0, 1):
        sends.append(Send("x+", ("X", 0, 0, h), ("X", 0, 3, h), xb, ox, h))
        sends.append(Send("x-", ("X", 0, 0, 1 - h), ("X", 0, 1, 1 - h), xb, ox, h))
    sends.append(Send("x+", ("X", 0, 3, 0), ("X", 0, 2, 0), xb, [("X", 0, 3, 0)], 0))
    sends.append(Send("x-", ("X", 0, 1, 1), ("X", 0, 2, 1), xb, [("X", 0, 1, 1)], 0))
    xkeys = [("own", "X"), ("X", 1, 0, 2)]
    for dx in (1, 3, 2):
        got = [("X", 0, dx, 0), ("X", 0, dx, 1)]
        sends.append(Send("s", ("X", 0, dx, 2), ("X", 1, dx, 2), 2 * xb, got, 0))
        xkeys += got + [("X", 1, dx, 2)]

    done = []
    for u in range(NZ):
        for n, first in (("A", "y"), ("B", "z")):
            tasks.append(Task("mm" + n, u, xkeys + unit_keys(n, first, u), [("mm", n, u)], 5))
            done.append(("mm", n, u))
    tasks.append(Task("silu", 0, done, [("H",)], 5))
    for u in range(NZ):
        dk = [("H",)] + unit_keys("DA", "y", u) + unit_keys("DB", "z", u)
        tasks.append(Task("dn", u, dk, [("P", u)], 5))
        sends.append(Send("s", ("S", u), ("S", u), 4 * 96 * 256 * 2, [("P", u)], 0))
        tasks.append(Task("red1", u, [("P", u), ("S", u)], [("T", u)], 4))
        sends.append(Send("x-", ("T", u, 0), ("R", u, 0), 48 * 512, [("T", u)], 0))
        sends.append(Send("x+", ("T", u, 1), ("R", u, 1), 48 * 512, [("T", u)], 0))
        tasks.append(Task("red2", u, [("T", u), ("R", u, 0), ("R", u, 1)], [("N", u)], 3))
        sends.append(Send("x-", ("N", u, 0), ("F", u, 0), 96 * 512, [("N", u)], 0))
        sends.append(Send("x+", ("N", u, 1), ("F", u, 1), 96 * 512, [("N", u)], 0))
        tasks.append(Task("fin", u, [("N", u), ("F", u, 0), ("F", u, 1)], [("O", u)], 2))
    return sends, tasks


def greedy(ops):
    known, free, order, t, left = {}, {}, [], 0.0, list(range(len(ops)))
    while left:
        best, soonest = None, None
        for i in left:
            o = ops[i]
            if any(k not in known for k in o.deps):
                continue
            at = max([known[k] for k in o.deps], default=0.0)
            if isinstance(o, Send):
                at = max(at, free.get(o.link, 0.0) - BACKLOG)
                rank = (0, o.prio, at)
            else:
                rank = (1, o.prio, at)
            if at <= t + 1e-9:
                if best is None or rank < best[0]:
                    best = (rank, i)
            elif soonest is None or at < soonest:
                soonest = at
        if best is None:
            t = soonest
            continue
        o = ops[best[1]]
        left.remove(best[1])
        order.append(best[1])
        if isinstance(o, Send):
            t += ISSUE
            rate, lat = (SIB, LAT_SIB) if o.link == "s" else (ICI, LAT)
            free[o.link] = max(free.get(o.link, 0.0), t) + o.nbytes / rate
            known[o.dst] = free[o.link] + lat
        else:
            t += o.dur
            for k in o.gives:
                known[k] = t
    return order


PLAN = (
    178, 0, 68, 97, 64, 32, 33, 96, 179, 129, 8, 4, 36, 9, 72, 128, 132, 40, 130, 73,
    100, 69, 1, 35, 99, 98, 34, 65, 5, 94, 131, 11, 93, 60, 12, 57, 41, 2, 53, 50,
    30, 10, 107, 27, 37, 90, 14, 135, 47, 134, 6, 75, 124, 133, 66, 78, 76, 43, 26, 24,
    61, 54, 79, 3, 13, 136, 58, 29, 51, 25, 92, 7, 31, 117, 48, 70, 137, 42, 62, 88,
    28, 183, 180, 23, 194, 38, 44, 18, 55, 95, 195, 59, 111, 20, 15, 52, 182, 16, 45, 63,
    19, 22, 21, 17, 39, 49, 114, 184, 81, 192, 185, 56, 104, 74, 71, 87, 125, 46, 112, 118,
    121, 181, 89, 67, 77, 193, 190, 80, 101, 186, 91, 191, 82, 189, 108, 115, 187, 188, 122, 105,
    196, 201, 143, 109, 84, 197, 138, 126, 225, 173, 119, 102, 221, 202, 144, 145, 123, 168, 205, 198,
    140, 148, 139, 113, 106, 83, 116, 226, 174, 110, 175, 85, 222, 169, 170, 206, 149, 150, 120, 127,
    86, 103, 203, 146, 147, 199, 141, 142, 217, 163, 227, 176, 177, 223, 209, 153, 218, 165, 164, 172,
    213, 158, 171, 207, 204, 210, 155, 200, 154, 214, 160, 152, 159, 151, 219, 166, 228, 167, 211, 224,
    157, 156, 215, 161, 162, 208, 220, 212, 216,
)
SENDS, TASKS = build()
OPS = SENDS + TASKS
ORDER = [OPS[i] for i in (PLAN or greedy(OPS))]


def number():
    links = ("y+", "y-", "z+", "z-", "x+", "x-", "s")
    count, sems = {}, {}
    for o in ORDER:
        if isinstance(o, Send):
            n = count.get(o.link, 0)
            count[o.link] = n + 1
            o.slot = links.index(o.link) * SLOTS + n % SLOTS
            group = o.dst[:2] if o.dst[0] in ("R", "F") else o.dst
            o.sem = sems.setdefault(group, len(sems))
    return len(links) * SLOTS, len(sems)


N_SEND, N_RECV = number()


def nt(a, b):
    return lax.dot_general(a, b, (((1,), (1,)), ((), ())), preferred_element_type=F32)


def kernel(
    tok_in, gain_in, gw_in, uw_in, gsc_in, usc_in, dw_in, dsc_in, out,
    tok, gain, gw, uw, gsc, usc, dw, dsc,
    xbuf, wa, wb, dbuf, acca, accb, hid, pown, ssend, srecv, tsend, rrecv, nsend, frecv,
    send_sems, recv_sems, in_sems,
):
    rep, fs, tp = lax.axis_index("rep"), lax.axis_index("fs"), lax.axis_index("tp")
    zlo, y = fs // NY, fs % NY
    zg = rep * NZ + zlo
    x, c = tp // 2, tp % 2

    def zn(step):
        to = (zg + step + 16) % 16
        return (to // NZ, (to % NZ) * NY + y, tp)

    def yn(step):
        return (rep, zlo * NY + (y + step + NY) % NY, tp)

    def xn(step):
        return (rep, fs, ((x + step + NX) % NX) * 2 + c)

    peer = {
        "z+": zn(1), "z-": zn(-1), "y+": yn(1), "y-": yn(-1),
        "x+": xn(1), "x-": xn(-1), "s": (rep, fs, x * 2 + 1 - c),
    }
    barrier = pltpu.get_barrier_semaphore()
    for p in peer.values():
        pl.semaphore_signal(barrier, inc=1, device_id=p, device_id_type=pl.DeviceIdType.MESH)

    loads = [
        pltpu.make_async_copy(a, b, in_sems.at[i])
        for i, (a, b) in enumerate(
            (
                (gw_in, gw), (uw_in, uw), (dw_in, dw), (tok_in, tok), (gain_in, gain),
                (gsc_in, gsc), (usc_in, usc), (dsc_in, dsc),
            )
        )
    ]
    for load in loads:
        load.start()

    yabs = [(y + dy) % NY for dy in range(NY)]
    parts = {
        "A": {"w": (0, 64), "l": (0, 32), "h": (32, 32)},
        "DA": {"w": (0, 128), "l": (0, 64), "h": (64, 64)},
        "DB": {"w": (128, 224), "l": (128, 112), "h": (240, 112)},
    }
    parts["B"] = parts["A"]

    def weight(name, dz, dy, part):
        at, n = parts[name][part]
        if name in ("A", "B"):
            rows = pl.ds(pl.multiple_of(yabs[dy] * 64 + at, 32), n)
            return (wa if name == "A" else wb).at[dz, rows, :]
        return dbuf.at[dz, yabs[dy], pl.ds(at, n), :]

    def place(key):
        name = key[0]
        if name in parts:
            return weight(*key)
        if name == "X":
            _, s, dx, h = key
            base = (s * 4 + dx) * ROWS
            return xbuf.at[:, pl.ds(base, ROWS) if h == 2 else pl.ds(base + h * 48, 48), :]
        if name == "T":
            return tsend.at[key[1], key[2]]
        if name == "R":
            return rrecv.at[key[1], key[2]]
        if name == "N":
            return nsend.at[key[1], key[2]]
        return frecv.at[key[1], key[2]]

    def copy(s, src, dst):
        return pltpu.make_async_remote_copy(
            src_ref=src, dst_ref=dst, send_sem=send_sems.at[s.slot], recv_sem=recv_sems.at[s.sem],
            device_id=peer[s.link], device_id_type=pl.DeviceIdType.MESH,
        )

    def outgoing(s):
        if s.src[0] == "S":
            return copy(s, ssend.at[s.src[1]], srecv.at[s.src[1]])
        if s.dst[0] in parts:
            name, dz, _, part = s.dst
            return copy(s, place(s.src), weight(name, dz, s.src[2], part))
        return copy(s, place(s.src), place(s.dst))

    by_dst = {s.dst: s for s in SENDS}
    waited = set()

    def arrive(key):
        if key not in by_dst:
            return
        s = by_dst[key]
        if s.sem in waited:
            return
        waited.add(s.sem)
        if key[0] == "S":
            ref = srecv.at[key[1]]
        elif key[0] in ("R", "F"):
            ref = (rrecv if key[0] == "R" else frecv).at[key[1]]
        else:
            ref = place(key)
        copy(s, ref, ref).wait_recv()

    first = {"A": True, "B": True}

    def run(o):
        u = o.unit
        if o.kind == "prep":
            for load in loads[:3]:
                load.wait()
            mine = pl.ds(pl.multiple_of(y * 64, 64), 64)
            g, v, dt = gw[...], uw[...], dw[...]
            wa[0, mine, :] = g[:, :WA].astype(BF16)
            wb[0, mine, pl.ds(0, WA)] = v[:, :WA].astype(BF16)
            mixed = jnp.concatenate([g[:, WA:], v[:, WA:]], axis=1)
            wb[0, mine, pl.ds(WA, 128)] = mixed.astype(BF16)
            for i in range(5):
                dbuf[0, y, pl.ds(i * 64, 64), :] = dt[:, i * 128 : (i + 1) * 128].astype(BF16)
            last = jnp.concatenate([dt[:32, WA:], dt[32:, WA:]], axis=1)
            dbuf[0, y, pl.ds(320, 32), :] = last.astype(BF16)
            pl.semaphore_wait(barrier, 7)
        elif o.kind == "norm":
            for load in loads[3:5]:
                load.wait()
            v = tok[...].astype(F32)
            r = lax.rsqrt(jnp.mean(v * v, axis=-1, keepdims=True) + 1e-06)
            n = (v * r * gain[...]).astype(BF16)
            for k in range(NZ):
                xbuf[(k - zlo + NZ) % NZ, pl.ds(0, ROWS), :] = n[:, k * 256 : (k + 1) * 256]
        elif o.kind in ("mmA", "mmB"):
            n = o.kind[2]
            w, acc = (wa, acca) if n == "A" else (wb, accb)
            start, first[n] = first[n], False

            part = jnp.dot(xbuf[u], w[u], preferred_element_type=F32)
            acc[...] = part if start else acc[...] + part
        elif o.kind == "silu":
            for load in loads[5:]:
                load.wait()
            gs, us = gsc[...].reshape(1, 704), usc[...].reshape(1, 704)
            mixed_scale = jnp.concatenate([gs[:, WA:], us[:, WA:]], axis=1)
            low = lax.broadcasted_iota(jnp.int32, (32, 128), 1) < 64

            @pl.loop(0, ALL_ROWS // 32)
            def _(i):
                rows = pl.ds(pl.multiple_of(i * 32, 32), 32)
                g = acca[rows, :] * gs[:, :WA]
                v = accb[rows, pl.ds(0, WA)] * us[:, :WA]
                hid[rows, pl.ds(0, WA)] = (g / (1.0 + jnp.exp(-g)) * v).astype(BF16)
                m = accb[rows, pl.ds(WA, 128)] * mixed_scale
                h = m / (1.0 + jnp.exp(-m)) * pltpu.roll(m, 64, 1)
                hid[rows, pl.ds(WA, 128)] = jnp.where(low, h, 0.0).astype(BF16)
        elif o.kind == "dn":
            tiles = [dbuf[u, :, pl.ds(i * 64, 64), :].reshape(256, 128) for i in range(5)]
            left = dbuf[u, :, pl.ds(320, 32), :]
            right = pltpu.roll(left.astype(F32).reshape(128, 128), 64, 1).astype(BF16)
            tiles.append(jnp.concatenate([left, right.reshape(4, 32, 128)], axis=1).reshape(256, 128))
            w = jnp.concatenate(tiles, axis=1)
            ssend[u] = nt(hid[pl.ds(384, 384), :], w).astype(BF16)
            pown[u] = nt(hid[pl.ds(0, 384), :], w)
        elif o.kind == "red1":
            q = pown[u] + srecv[u].astype(F32)
            pown[u] = q
            tsend[u, 0] = q[192:240].astype(BF16)
            tsend[u, 1] = q[240:288].astype(BF16)
        elif o.kind == "red2":
            r0, r1 = rrecv[u, 0].astype(F32), rrecv[u, 1].astype(F32)
            nsend[u, 0, pl.ds(0, 48), :] = (pown[u, pl.ds(288, 48), :] + r0).astype(BF16)
            nsend[u, 0, pl.ds(48, 48), :] = pown[u, pl.ds(336, 48), :].astype(BF16)
            nsend[u, 1, pl.ds(0, 48), :] = pown[u, pl.ds(96, 48), :].astype(BF16)
            nsend[u, 1, pl.ds(48, 48), :] = (pown[u, pl.ds(144, 48), :] + r1).astype(BF16)
        elif o.kind == "fin":
            total = pown[u, pl.ds(0, 96), :] + frecv[u, 0].astype(F32) + frecv[u, 1].astype(F32)
            cols = pl.ds(pl.multiple_of(((zlo + u) % NZ) * 256, 256), 256)
            out[:, cols] = (total * dsc[:, cols]).astype(BF16)

    sent = {}
    for o in ORDER:
        for key in o.deps:
            arrive(key)
        if isinstance(o, Send):
            if o.slot in sent:
                sent[o.slot].wait_send()
            sent[o.slot] = outgoing(o)
            sent[o.slot].start()
        else:
            run(o)
    for c_out in sent.values():
        c_out.wait_send()


def on_device(
    tokens, norm_gain, gate_weight, up_weight, gate_scale, up_scale, down_weight, down_scale
):
    hbm = pl.BlockSpec(memory_space=pl.ANY)
    vm = pl.BlockSpec(memory_space=pltpu.VMEM)
    return pl.pallas_call(
        kernel,
        out_shape=pltpu.VMEM((ROWS, D), BF16),
        in_specs=[hbm] * 8,
        out_specs=vm,
        scratch_shapes=[
            pltpu.VMEM((ROWS, D), BF16),
            pltpu.VMEM((1, D), F32),
            pltpu.VMEM((64, 704), F32),
            pltpu.VMEM((64, 704), F32),
            pltpu.VMEM((704,), F32),
            pltpu.VMEM((704,), F32),
            pltpu.VMEM((64, 704), F32),
            pltpu.VMEM((1, D), F32),
            pltpu.VMEM((8, ALL_ROWS, 256), BF16),
            pltpu.VMEM((8, 256, WA), BF16),
            pltpu.VMEM((8, 256, WB), BF16),
            pltpu.VMEM((8, 4, 352, 128), BF16),
            pltpu.VMEM((ALL_ROWS, WA), F32),
            pltpu.VMEM((ALL_ROWS, WB), F32),
            pltpu.VMEM((ALL_ROWS, DK), BF16),
            pltpu.VMEM((8, 384, 256), F32),
            pltpu.VMEM((8, 384, 256), BF16),
            pltpu.VMEM((8, 384, 256), BF16),
            pltpu.VMEM((8, 2, 48, 256), BF16),
            pltpu.VMEM((8, 2, 48, 256), BF16),
            pltpu.VMEM((8, 2, 96, 256), BF16),
            pltpu.VMEM((8, 2, 96, 256), BF16),
            pltpu.SemaphoreType.DMA((N_SEND,)),
            pltpu.SemaphoreType.DMA((N_RECV,)),
            pltpu.SemaphoreType.DMA((8,)),
        ],
        compiler_params=pltpu.CompilerParams(
            collective_id=0, has_side_effects=True, vmem_limit_bytes=60 * 1024 * 1024
        ),
    )(
        tokens, norm_gain[None], gate_weight, up_weight, gate_scale, up_scale,
        down_weight.T, down_scale[None],
    )


def solution(mesh):
    placed = (
        P(("rep", "fs", "tp"), None),
        P(),
        P("fs", "tp"),
        P("fs", "tp"),
        P("tp"),
        P("tp"),
        P("tp", "fs"),
        P(),
    )
    return jax.shard_map(
        on_device,
        mesh=mesh,
        in_specs=placed,
        out_specs=P(("rep", "fs", "tp"), None),
        check_vma=False,
    )
```

```python
import jax
import jax.numpy as jnp
from jax import lax
from jax.experimental import pallas as pl
from jax.experimental.pallas import tpu as pltpu
from jax.sharding import PartitionSpec as P

BF16 = jnp.bfloat16
F32 = jnp.float32
D = 2048
ROWS = 96
ALL_ROWS = 768
NZ, NY, NX = 8, 4, 4
WA, WB = 640, 768
DK = 768
LINKS = ("y+", "y-", "z+", "z-", "x+", "x-", "s")
SLOT_COUNT = {l: 5 for l in LINKS}

ICI, SIB = 45e3, 500e3
LAT, LAT_SIB = 2.3, 1.0
ISSUE, BACKLOG = 0.06, 1.5
COST = {
    "prep": 0.4, "norm": 0.5, "mmA": 0.35, "mmB": 0.4, "silu": 0.6, "dns": 0.22, "dno": 0.22,
    "red1": 0.15, "red2": 0.12, "fin": 0.12,
}


TURN = {("A", 0): 3, ("A", 1): 0, ("B", 0): 4, ("DA", 0): 3, ("DA", 1): 4, ("DB", 0): 2}


def ahead(name, dy):
    return tuple(range(1, TURN[name, dy] + 1))


def behind(name, dy):
    n = TURN[name, dy]
    return tuple(range(n - 1, 15)) if n else None


class Send:
    def __init__(self, link, src, dst, nbytes, deps, prio, only=None):
        self.link, self.src, self.dst, self.nbytes = link, src, dst, nbytes
        self.deps, self.prio, self.only = deps, prio, only
        self.slot = self.sem = None


class Task:
    def __init__(self, kind, unit, deps, gives, prio):
        self.kind, self.unit, self.deps, self.gives = kind, unit, deps, gives
        self.dur, self.prio = COST[kind], prio


def unit_keys(name, first, dz, dys=(0, 1, 2, 3)):
    keys = []
    for dy in dys:
        if (dz, dy) == (0, 0):
            keys.append(("own", name))
        elif (first == "y" and dz == 0 and dy == 2) or (first == "z" and dy == 0 and dz == 4):
            keys += [(name, dz, dy, "l"), (name, dz, dy, "h")]
        else:
            keys.append((name, dz, dy, "w"))
    return keys


def weight_sends(name, first, nbytes, p1, p2):
    sends = []

    def add(link, dz, dy, part, ddz, ddy, prio, only=None):
        deps = unit_keys(name, first, dz, (dy,))
        size = nbytes if part == "w" else nbytes // 2
        dst = (name, (dz + ddz) % NZ, (dy + ddy) % NY, part)
        sends.append(Send(link, (name, dz, dy, part), dst, size, deps, prio, only))

    if first == "y":
        add("y+", 0, 0, "w", 0, -1, p1)
        add("y-", 0, 0, "w", 0, 1, p1)
        add("y+", 0, 3, "l", 0, -1, p1)
        add("y-", 0, 1, "h", 0, 1, p1)
        for dy in range(4):
            for dz in (0, 7, 6, 5):
                if dz != 5 or dy in (0, 1):
                    add("z+", dz, dy, "w", -1, 0, p2, behind(name, dy) if dz == 5 else None)
            for dz in (0, 1, 2, 3):
                if dz != 3 or dy in (2, 3):
                    add("z-", dz, dy, "w", 1, 0, p2)
                else:
                    add("z-", dz, dy, "w", 1, 0, p2, ahead(name, dy))
    else:
        for dz in (0, 7, 6, 5):
            only = behind(name, 0) if dz == 5 else None
            add("z+", dz, 0, "l" if dz == 5 else "w", -1, 0, p1, only)
        for dz in (0, 1, 2, 3):
            add("z-", dz, 0, "h" if dz == 3 else "w", 1, 0, p1)
        add("z-", 3, 0, "l", 1, 0, p1, ahead(name, 0))
        for dz in range(NZ):
            add("y+", dz, 0, "w", 0, -1, p2)
            add("y-", dz, 0, "w", 0, 1, p2)
            if dz in (0, 6, 2, 4):
                add("y+", dz, 3, "w", 0, -1, p2 - 0.1)
            else:
                add("y-", dz, 1, "w", 0, 1, p2 - 0.1)
    return sends


def build():
    sends, tasks = [], []
    tasks.append(Task("prep", 0, [], [("own", n) for n in ("A", "B", "DA", "DB")], -2))
    tasks.append(Task("norm", 0, [], [("own", "X")], -1))
    sends += weight_sends("B", "z", 64 * WB * 2, 0, 2)
    sends += weight_sends("A", "y", 64 * WA * 2, 0, 2)
    sends += weight_sends("DB", "z", 224 * 256, 2.5, 3)
    sends += weight_sends("DA", "y", 128 * 256, 2.5, 3)

    xb = 48 * D * 2
    ox = [("own", "X")]
    sends.append(Send("s", ("X", 0, 0, 2), ("X", 1, 0, 2), 2 * xb, ox, 0))
    for h in (0, 1):
        sends.append(Send("x+", ("X", 0, 0, h), ("X", 0, 3, h), xb, ox, h))
        sends.append(Send("x-", ("X", 0, 0, 1 - h), ("X", 0, 1, 1 - h), xb, ox, h))
    sends.append(Send("x+", ("X", 0, 3, 0), ("X", 0, 2, 0), xb, [("X", 0, 3, 0)], 0))
    sends.append(Send("x-", ("X", 0, 1, 1), ("X", 0, 2, 1), xb, [("X", 0, 1, 1)], 0))
    xkeys = [("own", "X"), ("X", 1, 0, 2)]
    for dx in (1, 3, 2):
        got = [("X", 0, dx, 0), ("X", 0, dx, 1)]
        sends.append(Send("s", ("X", 0, dx, 2), ("X", 1, dx, 2), 2 * xb, got, 0))
        xkeys += got + [("X", 1, dx, 2)]

    done = []
    for u in range(NZ):
        for n, first in (("A", "y"), ("B", "z")):
            tasks.append(Task("mm" + n, u, xkeys + unit_keys(n, first, u), [("mm", n, u)], 5))
            done.append(("mm", n, u))
    tasks.append(Task("silu", 1, done, [("H", 1)], 5))
    tasks.append(Task("silu", 0, done, [("H", 0)], 5))
    for u in range(NZ):
        dk = unit_keys("DA", "y", u) + unit_keys("DB", "z", u)
        tasks.append(Task("dns", u, [("H", 1)] + dk, [("PS", u)], 4.5))
        tasks.append(Task("dno", u, [("H", 0)] + dk, [("P", u)], 5))
        sends.append(Send("s", ("S", u), ("S", u), 4 * 96 * 256 * 2, [("PS", u)], 0))
        tasks.append(Task("red1", u, [("P", u), ("S", u)], [("T", u)], 4))
        sends.append(Send("x-", ("T", u, 0), ("R", u, 0), 48 * 512, [("T", u)], 0))
        sends.append(Send("x+", ("T", u, 1), ("R", u, 1), 48 * 512, [("T", u)], 0))
        tasks.append(Task("red2", u, [("T", u), ("R", u, 0), ("R", u, 1)], [("N", u)], 3))
        sends.append(Send("x-", ("N", u, 0), ("F", u, 0), 96 * 512, [("N", u)], 0))
        sends.append(Send("x+", ("N", u, 1), ("F", u, 1), 96 * 512, [("N", u)], 0))
        tasks.append(Task("fin", u, [("N", u), ("F", u, 0), ("F", u, 1)], [("O", u)], 2))
    return sends, tasks


def greedy(ops):
    known, free, order, t, left = {}, {}, [], 0.0, list(range(len(ops)))
    missing = {}
    for o in ops:
        for k in [o.dst] if isinstance(o, Send) else o.gives:
            missing[k] = missing.get(k, 0) + 1
    while left:
        best, soonest = None, None
        for i in left:
            o = ops[i]
            if any(missing[k] for k in o.deps):
                continue
            at = max([known[k] for k in o.deps], default=0.0)
            if isinstance(o, Send):
                at = max(at, free.get(o.link, 0.0) - BACKLOG)
                rank = (0, o.prio, at)
            else:
                rank = (1, o.prio, at)
            if at <= t + 1e-9:
                if best is None or rank < best[0]:
                    best = (rank, i)
            elif soonest is None or at < soonest:
                soonest = at
        if best is None:
            t = soonest
            continue
        o = ops[best[1]]
        left.remove(best[1])
        order.append(best[1])
        if isinstance(o, Send):
            t += ISSUE
            rate, lat = (SIB, LAT_SIB) if o.link == "s" else (ICI, LAT)
            free[o.link] = max(free.get(o.link, 0.0), t) + o.nbytes / rate
            known[o.dst] = max(known.get(o.dst, 0.0), free[o.link] + lat)
            missing[o.dst] -= 1
        else:
            t += o.dur
            for k in o.gives:
                known[k] = t
                missing[k] -= 1
    return order


PLAN = (
    184, 0, 4, 33, 34, 76, 9, 71, 185, 41, 67, 134, 37, 135, 136, 101, 10, 100, 45, 36,
    13, 35, 5, 63, 112, 12, 49, 72, 31, 138, 30, 1, 103, 53, 79, 60, 68, 14, 6, 139,
    15, 98, 56, 64, 42, 16, 2, 46, 102, 27, 80, 137, 7, 140, 8, 11, 82, 19, 73, 50,
    61, 32, 17, 38, 57, 24, 29, 3, 25, 69, 141, 120, 104, 99, 54, 43, 47, 142, 65, 75,
    62, 22, 21, 143, 123, 26, 28, 187, 201, 51, 189, 86, 188, 58, 18, 92, 39, 186, 44, 55,
    94, 130, 20, 191, 81, 116, 127, 190, 66, 77, 197, 23, 198, 97, 83, 48, 59, 85, 95, 78,
    40, 108, 74, 105, 84, 70, 131, 52, 200, 113, 87, 199, 192, 96, 121, 128, 93, 196, 124, 195,
    193, 117, 194, 202, 109, 239, 179, 106, 209, 149, 132, 88, 203, 125, 114, 91, 240, 122, 241, 181,
    180, 118, 204, 144, 129, 89, 210, 110, 214, 154, 205, 211, 151, 150, 234, 174, 133, 206, 146, 145,
    126, 215, 216, 156, 155, 90, 235, 119, 242, 183, 182, 219, 111, 159, 236, 176, 175, 107, 212, 153,
    152, 115, 220, 221, 161, 160, 207, 148, 147, 229, 169, 217, 158, 157, 224, 164, 230, 225, 231, 170,
    171, 226, 166, 165, 243, 237, 177, 178, 222, 208, 213, 163, 162, 232, 172, 173, 218, 227, 168, 167,
    223, 233, 238, 228,
)
SENDS, TASKS = build()
OPS = SENDS + TASKS
ORDER = [OPS[i] for i in (PLAN or greedy(OPS))]


def number():
    base = {l: sum(SLOT_COUNT[m] for m in LINKS[:i]) for i, l in enumerate(LINKS)}
    count, sems = {}, {}
    for o in ORDER:
        if isinstance(o, Send):
            if o.only != ():
                n = count.get(o.link, 0)
                count[o.link] = n + 1
                o.slot = base[o.link] + n % SLOT_COUNT[o.link]
            users = tuple(i for i, q in enumerate(ORDER) if o.dst in q.deps)
            o.sem = sems.setdefault(users, len(sems))
    return sum(SLOT_COUNT.values()), len(sems)


N_SEND, N_RECV = number()


def silu(v):
    return 0.5 * v * (1.0 + jnp.tanh(0.5 * v))


def nt(a, b):
    return lax.dot_general(a, b, (((1,), (1,)), ((), ())), preferred_element_type=F32)


def kernel(
    tok_in, gain_in, gw_in, uw_in, gsc_in, usc_in, dw_in, dsc_in, out,
    tok, gain, gw, uw, gsc, usc, dw, dsc,
    xbuf, wa, wb, dbuf, acca, accb, hid, pown, ssend, srecv, tsend, rrecv, nsend, frecv,
    send_sems, recv_sems, in_sems,
):
    rep, fs, tp = lax.axis_index("rep"), lax.axis_index("fs"), lax.axis_index("tp")
    zlo, y = fs // NY, fs % NY
    zg = rep * NZ + zlo
    x, c = tp // 2, tp % 2

    def zn(step):
        to = (zg + step + 16) % 16
        return (to // NZ, (to % NZ) * NY + y, tp)

    def yn(step):
        return (rep, zlo * NY + (y + step + NY) % NY, tp)

    def xn(step):
        return (rep, fs, ((x + step + NX) % NX) * 2 + c)

    peer = {
        "z+": zn(1), "z-": zn(-1), "y+": yn(1), "y-": yn(-1),
        "x+": xn(1), "x-": xn(-1), "s": (rep, fs, x * 2 + 1 - c),
    }
    barrier = pltpu.get_barrier_semaphore()
    for p in peer.values():
        pl.semaphore_signal(barrier, inc=1, device_id=p, device_id_type=pl.DeviceIdType.MESH)

    loads = [
        pltpu.make_async_copy(a, b, in_sems.at[i])
        for i, (a, b) in enumerate(
            (
                (gw_in, gw), (uw_in, uw), (dw_in, dw), (tok_in, tok), (gain_in, gain),
                (gsc_in, gsc), (usc_in, usc), (dsc_in, dsc),
            )
        )
    ]
    for load in loads:
        load.start()

    yabs = [(y + dy) % NY for dy in range(NY)]
    parts = {
        "A": {"w": (0, 64), "l": (0, 32), "h": (32, 32)},
        "DA": {"w": (0, 128), "l": (0, 64), "h": (64, 64)},
        "DB": {"w": (128, 224), "l": (128, 112), "h": (240, 112)},
    }
    parts["B"] = parts["A"]

    def weight(name, dz, dy, part):
        at, n = parts[name][part]
        if name in ("A", "B"):
            rows = pl.ds(pl.multiple_of(yabs[dy] * 64 + at, 32), n)
            return (wa if name == "A" else wb).at[dz, rows, :]
        return dbuf.at[dz, yabs[dy], pl.ds(at, n), :]

    def place(key):
        name = key[0]
        if name in parts:
            return weight(*key)
        if name == "X":
            _, s, dx, h = key
            base = (s * 4 + dx) * ROWS
            return xbuf.at[:, pl.ds(base, ROWS) if h == 2 else pl.ds(base + h * 48, 48), :]
        if name == "T":
            return tsend.at[key[1], key[2]]
        if name == "R":
            return rrecv.at[key[1], key[2]]
        if name == "N":
            return nsend.at[key[1], key[2]]
        return frecv.at[key[1], key[2]]

    def copy(s, src, dst):
        return pltpu.make_async_remote_copy(
            src_ref=src, dst_ref=dst, send_sem=send_sems.at[s.slot], recv_sem=recv_sems.at[s.sem],
            device_id=peer[s.link], device_id_type=pl.DeviceIdType.MESH,
        )

    def outgoing(s):
        if s.src[0] == "S":
            return copy(s, ssend.at[s.src[1]], srecv.at[s.src[1]])
        if s.dst[0] in parts:
            name, dz, _, part = s.dst
            return copy(s, place(s.src), weight(name, dz, s.src[2], part))
        return copy(s, place(s.src), place(s.dst))

    by_dst = {q.dst: q for q in SENDS if q.only != ()}
    waited = set()

    def arrive(key):
        if key not in by_dst:
            return
        s = by_dst[key]
        if s.sem in waited:
            return
        waited.add(s.sem)
        total = sum({q.dst: q.nbytes for q in SENDS if q.sem == s.sem}.values())
        tall = [k for k in range(1, 9) if total % (8192 * k) == 0 and total // (512 * k) <= ALL_ROWS]
        if total % 8192:
            ref = place(key)
        else:
            ref = xbuf.at[pl.ds(0, tall[0]), pl.ds(0, total // (512 * tall[0])), :]
        copy(s, ref, ref).wait_recv()

    first = {"A": True, "B": True}

    def run(o):
        u = o.unit
        if o.kind == "prep":
            for load in loads[:3]:
                load.wait()
            mine = pl.ds(pl.multiple_of(y * 64, 64), 64)
            g, v, dt = gw[...], uw[...], dw[...]
            wa[0, mine, :] = g[:, :WA].astype(BF16)
            wb[0, mine, pl.ds(0, WA)] = v[:, :WA].astype(BF16)
            mixed = jnp.concatenate([g[:, WA:], v[:, WA:]], axis=1)
            wb[0, mine, pl.ds(WA, 128)] = mixed.astype(BF16)
            for i in range(5):
                dbuf[0, y, pl.ds(i * 64, 64), :] = dt[:, i * 128 : (i + 1) * 128].astype(BF16)
            last = jnp.concatenate([dt[:32, WA:], dt[32:, WA:]], axis=1)
            dbuf[0, y, pl.ds(320, 32), :] = last.astype(BF16)
            pl.semaphore_wait(barrier, 7)
        elif o.kind == "norm":
            for load in loads[3:5]:
                load.wait()
            v = tok[...].astype(F32)
            r = lax.rsqrt(jnp.mean(v * v, axis=-1, keepdims=True) + 1e-06)
            n = (v * r * gain[...]).astype(BF16)
            for k in range(NZ):
                xbuf[(k - zlo + NZ) % NZ, pl.ds(0, ROWS), :] = n[:, k * 256 : (k + 1) * 256]
        elif o.kind in ("mmA", "mmB"):
            n = o.kind[2]
            w, acc = (wa, acca) if n == "A" else (wb, accb)
            start, first[n] = first[n], False

            part = jnp.dot(xbuf[u], w[u], preferred_element_type=F32)
            acc[...] = part if start else acc[...] + part
        elif o.kind == "silu":
            if u == 1:
                for load in loads[5:]:
                    load.wait()
            gs, us = gsc[...].reshape(1, 704), usc[...].reshape(1, 704)
            mixed_scale = jnp.concatenate([gs[:, WA:], us[:, WA:]], axis=1)
            low = lax.broadcasted_iota(jnp.int32, (32, 128), 1) < 64

            @pl.loop(0, 384 // 32)
            def _(i):
                rows = pl.ds(pl.multiple_of(u * 384 + i * 32, 32), 32)
                g = acca[rows, :] * gs[:, :WA]
                v = accb[rows, pl.ds(0, WA)] * us[:, :WA]
                hid[rows, pl.ds(0, WA)] = (silu(g) * v).astype(BF16)
                m = accb[rows, pl.ds(WA, 128)] * mixed_scale
                h = silu(m) * pltpu.roll(m, 64, 1)
                hid[rows, pl.ds(WA, 128)] = jnp.where(low, h, 0.0).astype(BF16)
        elif o.kind in ("dns", "dno"):
            tiles = [dbuf[u, :, pl.ds(i * 64, 64), :].reshape(256, 128) for i in range(5)]
            left = dbuf[u, :, pl.ds(320, 32), :]
            right = pltpu.roll(left.astype(F32).reshape(128, 128), 64, 1).astype(BF16)
            tiles.append(jnp.concatenate([left, right.reshape(4, 32, 128)], axis=1).reshape(256, 128))
            w = jnp.concatenate(tiles, axis=1)
            if o.kind == "dns":
                ssend[u] = nt(hid[pl.ds(384, 384), :], w).astype(BF16)
            else:
                pown[u] = nt(hid[pl.ds(0, 384), :], w)
        elif o.kind == "red1":
            q = pown[u] + srecv[u].astype(F32)
            pown[u] = q
            tsend[u, 0] = q[192:240].astype(BF16)
            tsend[u, 1] = q[240:288].astype(BF16)
        elif o.kind == "red2":
            r0, r1 = rrecv[u, 0].astype(F32), rrecv[u, 1].astype(F32)
            nsend[u, 0, pl.ds(0, 48), :] = (pown[u, pl.ds(288, 48), :] + r0).astype(BF16)
            nsend[u, 0, pl.ds(48, 48), :] = pown[u, pl.ds(336, 48), :].astype(BF16)
            nsend[u, 1, pl.ds(0, 48), :] = pown[u, pl.ds(96, 48), :].astype(BF16)
            nsend[u, 1, pl.ds(48, 48), :] = (pown[u, pl.ds(144, 48), :] + r1).astype(BF16)
        elif o.kind == "fin":
            total = pown[u, pl.ds(0, 96), :] + frecv[u, 0].astype(F32) + frecv[u, 1].astype(F32)
            cols = pl.ds(pl.multiple_of(((zlo + u) % NZ) * 256, 256), 256)
            out[:, cols] = (total * dsc[:, cols]).astype(BF16)

    def active(s):
        return (zg >= s.only[0]) & (zg <= s.only[-1])

    def begin(s):
        if s.only is None:
            outgoing(s).start()
        else:
            pl.when(active(s))(lambda: outgoing(s).start())

    def finish(s):
        if s.only is None:
            outgoing(s).wait_send()
        else:
            pl.when(active(s))(lambda: outgoing(s).wait_send())

    sent = {}
    for o in ORDER:
        if isinstance(o, Send) and o.only == ():
            continue
        for key in o.deps:
            arrive(key)
        if isinstance(o, Send):
            if o.slot in sent:
                finish(sent[o.slot])
            sent[o.slot] = o
            begin(o)
        else:
            run(o)
    for o in sent.values():
        finish(o)


def on_device(
    tokens, norm_gain, gate_weight, up_weight, gate_scale, up_scale, down_weight, down_scale
):
    hbm = pl.BlockSpec(memory_space=pl.ANY)
    vm = pl.BlockSpec(memory_space=pltpu.VMEM)
    return pl.pallas_call(
        kernel,
        out_shape=pltpu.VMEM((ROWS, D), BF16),
        in_specs=[hbm] * 8,
        out_specs=vm,
        scratch_shapes=[
            pltpu.VMEM((ROWS, D), BF16),
            pltpu.VMEM((1, D), F32),
            pltpu.VMEM((64, 704), F32),
            pltpu.VMEM((64, 704), F32),
            pltpu.VMEM((704,), F32),
            pltpu.VMEM((704,), F32),
            pltpu.VMEM((64, 704), F32),
            pltpu.VMEM((1, D), F32),
            pltpu.VMEM((8, ALL_ROWS, 256), BF16),
            pltpu.VMEM((8, 256, WA), BF16),
            pltpu.VMEM((8, 256, WB), BF16),
            pltpu.VMEM((8, 4, 352, 128), BF16),
            pltpu.VMEM((ALL_ROWS, WA), F32),
            pltpu.VMEM((ALL_ROWS, WB), F32),
            pltpu.VMEM((ALL_ROWS, DK), BF16),
            pltpu.VMEM((8, 384, 256), F32),
            pltpu.VMEM((8, 384, 256), BF16),
            pltpu.VMEM((8, 384, 256), BF16),
            pltpu.VMEM((8, 2, 48, 256), BF16),
            pltpu.VMEM((8, 2, 48, 256), BF16),
            pltpu.VMEM((8, 2, 96, 256), BF16),
            pltpu.VMEM((8, 2, 96, 256), BF16),
            pltpu.SemaphoreType.DMA((N_SEND,)),
            pltpu.SemaphoreType.DMA((N_RECV,)),
            pltpu.SemaphoreType.DMA((8,)),
        ],
        compiler_params=pltpu.CompilerParams(
            collective_id=0, has_side_effects=True, vmem_limit_bytes=60 * 1024 * 1024
        ),
    )(
        tokens, norm_gain[None], gate_weight, up_weight, gate_scale, up_scale,
        down_weight.T, down_scale[None],
    )


def solution(mesh):
    placed = (
        P(("rep", "fs", "tp"), None),
        P(),
        P("fs", "tp"),
        P("fs", "tp"),
        P("tp"),
        P("tp"),
        P("tp", "fs"),
        P(),
    )
    return jax.shard_map(
        on_device,
        mesh=mesh,
        in_specs=placed,
        out_specs=P(("rep", "fs", "tp"), None),
        check_vma=False,
    )
```

```python
import jax
import jax.numpy as jnp
from jax import lax
from jax.experimental import pallas as pl
from jax.experimental.pallas import tpu as pltpu
from jax.sharding import PartitionSpec as P

BF16 = jnp.bfloat16
F32 = jnp.float32
D = 2048
ROWS = 96
ALL_ROWS = 768
NZ, NY, NX = 8, 4, 4
WA, WB = 640, 768
DK = 768
LINKS = ("y+", "y-", "z+", "z-", "x+", "x-", "s")
SLOT_COUNT = {l: 5 for l in LINKS}

ICI, SIB = 45e3, 500e3
LAT, LAT_SIB = 2.3, 1.0
ISSUE, BACKLOG = 0.06, 1.5
COST = {
    "prep": 0.4, "norm": 0.5, "mmA": 0.35, "mmB": 0.4, "silu": 0.6, "dns": 0.22, "dno": 0.22,
    "red1": 0.15, "red2": 0.12, "fin": 0.12,
}


TURN = {("A", 0): 0, ("A", 1): 3, ("B", 0): 2, ("DA", 0): 4, ("DA", 1): 4, ("DB", 0): 0}

SPREAD = {("A", 7): 0, ("A", 6): 0, ("A", 5): 0, ("DA", 7): 0, ("DA", 6): 0, ("DA", 5): 0}


def ahead(name, dy):
    return tuple(range(1, TURN[name, dy] + 1))


def behind(n):
    return tuple(range(n - 1, 15)) if n else None


class Send:
    def __init__(self, link, src, dst, nbytes, deps, prio, only=None):
        self.link, self.src, self.dst, self.nbytes = link, src, dst, nbytes
        self.deps, self.prio, self.only = deps, prio, only
        self.slot = self.sem = None


class Task:
    def __init__(self, kind, unit, deps, gives, prio):
        self.kind, self.unit, self.deps, self.gives = kind, unit, deps, gives
        self.dur, self.prio = COST[kind], prio


def unit_keys(name, first, dz, dys=(0, 1, 2, 3)):
    keys = []
    for dy in dys:
        if (dz, dy) == (0, 0):
            keys.append(("own", name))
        elif (first == "y" and dz == 0 and dy == 2) or (first == "z" and dy == 0 and dz == 4):
            keys += [(name, dz, dy, "l"), (name, dz, dy, "h")]
        else:
            keys.append((name, dz, dy, "w"))
    return keys


def weight_sends(name, first, nbytes, p1, p2):
    sends = []

    def add(link, dz, dy, part, ddz, ddy, prio, only=None):
        deps = unit_keys(name, first, dz, (dy,))
        size = nbytes if part == "w" else nbytes // 2
        dst = (name, (dz + ddz) % NZ, (dy + ddy) % NY, part)
        sends.append(Send(link, (name, dz, dy, part), dst, size, deps, prio, only))

    if first == "y":
        add("y+", 0, 0, "w", 0, -1, p1)
        add("y-", 0, 0, "w", 0, 1, p1)
        add("y+", 0, 3, "l", 0, -1, p1)
        add("y-", 0, 1, "h", 0, 1, p1)
        for dz in (7, 6, 5):
            spread = tuple(range(SPREAD[name, dz]))
            add("y+", dz, 0, "w", 0, -1, p2, spread)
            add("y-", dz, 0, "w", 0, 1, p2, spread)
            add("y+", dz, 3, "w", 0, -1, p2, spread)
        for dy in range(4):
            for dz in (0, 7, 6, 5):
                if dz != 5 or dy in (0, 1):
                    if dz == 5:
                        only = behind(TURN[name, dy])
                    else:
                        only = behind(SPREAD[name, (dz - 1) % NZ]) if dy else None
                    add("z+", dz, dy, "w", -1, 0, p2, only)
            for dz in (0, 1, 2, 3):
                if dz != 3 or dy in (2, 3):
                    add("z-", dz, dy, "w", 1, 0, p2)
                else:
                    add("z-", dz, dy, "w", 1, 0, p2, ahead(name, dy))
    else:
        for dz in (0, 7, 6, 5):
            only = behind(TURN[name, 0]) if dz == 5 else None
            add("z+", dz, 0, "l" if dz == 5 else "w", -1, 0, p1, only)
        for dz in (0, 1, 2, 3):
            add("z-", dz, 0, "h" if dz == 3 else "w", 1, 0, p1)
        add("z-", 3, 0, "l", 1, 0, p1, ahead(name, 0))
        for dz in range(NZ):
            add("y+", dz, 0, "w", 0, -1, p2)
            add("y-", dz, 0, "w", 0, 1, p2)
            if dz in (0, 6, 2, 4):
                add("y+", dz, 3, "w", 0, -1, p2 - 0.1)
            else:
                add("y-", dz, 1, "w", 0, 1, p2 - 0.1)
    return sends


def build():
    sends, tasks = [], []
    tasks.append(Task("prep", 0, [], [("own", n) for n in ("A", "B", "DA", "DB")], -2))
    tasks.append(Task("norm", 0, [], [("own", "X")], -1))
    sends += weight_sends("B", "z", 64 * WB * 2, 0, 2)
    sends += weight_sends("A", "y", 64 * WA * 2, 0, 2)
    sends += weight_sends("DB", "z", 256 * 256, 2.5, 3)
    sends += weight_sends("DA", "y", 96 * 256, 2.5, 3)

    xb = 48 * D * 2
    ox = [("own", "X")]
    sends.append(Send("s", ("X", 0, 0, 2), ("X", 1, 0, 2), 2 * xb, ox, 0))
    for h in (0, 1):
        sends.append(Send("x+", ("X", 0, 0, h), ("X", 0, 3, h), xb, ox, h))
        sends.append(Send("x-", ("X", 0, 0, 1 - h), ("X", 0, 1, 1 - h), xb, ox, h))
    sends.append(Send("x+", ("X", 0, 3, 0), ("X", 0, 2, 0), xb, [("X", 0, 3, 0)], 0))
    sends.append(Send("x-", ("X", 0, 1, 1), ("X", 0, 2, 1), xb, [("X", 0, 1, 1)], 0))
    xkeys = [("own", "X"), ("X", 1, 0, 2)]
    for dx in (1, 3, 2):
        got = [("X", 0, dx, 0), ("X", 0, dx, 1)]
        sends.append(Send("s", ("X", 0, dx, 2), ("X", 1, dx, 2), 2 * xb, got, 0))
        xkeys += got + [("X", 1, dx, 2)]

    done = []
    for u in range(NZ):
        for n, first in (("A", "y"), ("B", "z")):
            tasks.append(Task("mm" + n, u, xkeys + unit_keys(n, first, u), [("mm", n, u)], 5))
            done.append(("mm", n, u))
    tasks.append(Task("silu", 1, done, [("H", 1)], 5))
    tasks.append(Task("silu", 0, done, [("H", 0)], 5))
    for u in range(NZ):
        dk = unit_keys("DA", "y", u) + unit_keys("DB", "z", u)
        tasks.append(Task("dns", u, [("H", 1)] + dk, [("PS", u)], 4.5))
        tasks.append(Task("dno", u, [("H", 0)] + dk, [("P", u)], 5))
        sends.append(Send("s", ("S", u), ("S", u), 4 * 96 * 256 * 2, [("PS", u)], 0))
        tasks.append(Task("red1", u, [("P", u), ("S", u)], [("T", u)], 4))
        sends.append(Send("x-", ("T", u, 0), ("R", u, 0), 48 * 512, [("T", u)], 0))
        sends.append(Send("x+", ("T", u, 1), ("R", u, 1), 48 * 512, [("T", u)], 0))
        tasks.append(Task("red2", u, [("T", u), ("R", u, 0), ("R", u, 1)], [("N", u)], 3))
        sends.append(Send("x-", ("N", u, 0), ("F", u, 0), 96 * 512, [("N", u)], 0))
        sends.append(Send("x+", ("N", u, 1), ("F", u, 1), 96 * 512, [("N", u)], 0))
        tasks.append(Task("fin", u, [("N", u), ("F", u, 0), ("F", u, 1)], [("O", u)], 2))
    return sends, tasks


def greedy(ops):
    known, free, order, t, left = {}, {}, [], 0.0, list(range(len(ops)))
    missing = {}
    for o in ops:
        for k in [o.dst] if isinstance(o, Send) else o.gives:
            missing[k] = missing.get(k, 0) + 1
    while left:
        best, soonest = None, None
        for i in left:
            o = ops[i]
            if any(missing[k] for k in o.deps):
                continue
            at = max([known[k] for k in o.deps], default=0.0)
            if isinstance(o, Send):
                at = max(at, free.get(o.link, 0.0) - BACKLOG)
                rank = (0, o.prio, at)
            else:
                rank = (1, o.prio, at)
            if at <= t + 1e-9:
                if best is None or rank < best[0]:
                    best = (rank, i)
            elif soonest is None or at < soonest:
                soonest = at
        if best is None:
            t = soonest
            continue
        o = ops[best[1]]
        left.remove(best[1])
        order.append(best[1])
        if isinstance(o, Send):
            t += ISSUE
            rate, lat = (SIB, LAT_SIB) if o.link == "s" else (ICI, LAT)
            free[o.link] = max(free.get(o.link, 0.0), t) + o.nbytes / rate
            known[o.dst] = max(known.get(o.dst, 0.0), free[o.link] + lat)
            missing[o.dst] -= 1
        else:
            t += o.dur
            for k in o.gives:
                known[k] = t
                missing[k] -= 1
    return order


PLAN = (
    202, 0, 4, 33, 34, 76, 203, 9, 126, 10, 154, 80, 50, 46, 86, 155, 85, 36, 54, 5,
    72, 58, 12, 110, 153, 1, 31, 109, 69, 35, 88, 89, 81, 152, 77, 15, 11, 6, 158, 16,
    38, 13, 65, 37, 62, 73, 157, 2, 51, 27, 156, 59, 28, 32, 70, 55, 134, 160, 111, 47,
    17, 7, 39, 18, 91, 19, 29, 40, 42, 161, 107, 66, 3, 78, 159, 74, 63, 8, 122, 14,
    30, 41, 25, 112, 56, 20, 113, 60, 48, 43, 145, 148, 21, 130, 103, 67, 90, 205, 24, 82,
    207, 218, 71, 204, 216, 61, 26, 64, 138, 22, 52, 23, 44, 106, 93, 209, 149, 114, 53, 141,
    49, 57, 108, 75, 131, 87, 219, 105, 45, 92, 211, 68, 115, 206, 95, 217, 123, 127, 79, 215,
    117, 208, 139, 83, 146, 214, 210, 101, 142, 104, 213, 135, 212, 116, 220, 227, 167, 124, 132, 150,
    221, 257, 84, 97, 197, 143, 232, 172, 118, 140, 128, 228, 229, 168, 169, 120, 96, 147, 136, 94,
    222, 162, 100, 258, 259, 199, 198, 233, 234, 174, 173, 102, 223, 224, 163, 164, 98, 151, 99, 230,
    171, 170, 129, 252, 192, 119, 144, 253, 260, 201, 200, 125, 137, 237, 177, 235, 176, 133, 175, 254,
    193, 121, 225, 194, 238, 247, 187, 239, 179, 178, 165, 166, 242, 182, 231, 248, 249, 188, 189, 243,
    244, 184, 183, 255, 196, 195, 236, 240, 180, 181, 261, 226, 250, 191, 190, 245, 185, 186, 251, 256,
    241, 246,
)
SENDS, TASKS = build()
OPS = SENDS + TASKS
ORDER = [OPS[i] for i in (PLAN or greedy(OPS))]


def number():
    base = {l: sum(SLOT_COUNT[m] for m in LINKS[:i]) for i, l in enumerate(LINKS)}
    count, sems = {}, {}
    for o in ORDER:
        if isinstance(o, Send):
            if o.only != ():
                n = count.get(o.link, 0)
                count[o.link] = n + 1
                o.slot = base[o.link] + n % SLOT_COUNT[o.link]
            users = tuple(i for i, q in enumerate(ORDER) if o.dst in q.deps)
            o.sem = sems.setdefault(users, len(sems))
    return sum(SLOT_COUNT.values()), len(sems)


N_SEND, N_RECV = number()


def silu(v):
    return 0.5 * v * (1.0 + jnp.tanh(0.5 * v))


def nt(a, b):
    return lax.dot_general(a, b, (((1,), (1,)), ((), ())), preferred_element_type=F32)


def kernel(
    tok_in, gain_in, gw_in, uw_in, gsc_in, usc_in, dw_in, dsc_in, out,
    tok, gain, gw, uw, gsc, usc, dw, dsc,
    xbuf, wa, wb, dbuf, acca, accb, hid, pown, ssend, srecv, tsend, rrecv, nsend, frecv,
    send_sems, recv_sems, in_sems,
):
    rep, fs, tp = lax.axis_index("rep"), lax.axis_index("fs"), lax.axis_index("tp")
    zlo, y = fs // NY, fs % NY
    zg = rep * NZ + zlo
    x, c = tp // 2, tp % 2

    def zn(step):
        to = (zg + step + 16) % 16
        return (to // NZ, (to % NZ) * NY + y, tp)

    def yn(step):
        return (rep, zlo * NY + (y + step + NY) % NY, tp)

    def xn(step):
        return (rep, fs, ((x + step + NX) % NX) * 2 + c)

    peer = {
        "z+": zn(1), "z-": zn(-1), "y+": yn(1), "y-": yn(-1),
        "x+": xn(1), "x-": xn(-1), "s": (rep, fs, x * 2 + 1 - c),
    }
    barrier = pltpu.get_barrier_semaphore()
    for p in peer.values():
        pl.semaphore_signal(barrier, inc=1, device_id=p, device_id_type=pl.DeviceIdType.MESH)

    loads = [
        pltpu.make_async_copy(a, b, in_sems.at[i])
        for i, (a, b) in enumerate(
            (
                (gw_in, gw), (uw_in, uw), (dw_in, dw), (tok_in, tok), (gain_in, gain),
                (gsc_in, gsc), (usc_in, usc), (dsc_in, dsc),
            )
        )
    ]
    for load in loads:
        load.start()

    yabs = [(y + dy) % NY for dy in range(NY)]
    parts = {
        "A": {"w": (0, 64), "l": (0, 32), "h": (32, 32)},
        "DA": {"w": (0, 96), "l": (0, 48), "h": (48, 48)},
        "DB": {"w": (96, 256), "l": (96, 128), "h": (224, 128)},
    }
    parts["B"] = parts["A"]

    def weight(name, dz, dy, part):
        at, n = parts[name][part]
        if name in ("A", "B"):
            rows = pl.ds(pl.multiple_of(yabs[dy] * 64 + at, 32), n)
            return (wa if name == "A" else wb).at[dz, rows, :]
        return dbuf.at[dz, yabs[dy], pl.ds(at, n), :]

    def place(key):
        name = key[0]
        if name in parts:
            return weight(*key)
        if name == "X":
            _, s, dx, h = key
            base = (s * 4 + dx) * ROWS
            return xbuf.at[:, pl.ds(base, ROWS) if h == 2 else pl.ds(base + h * 48, 48), :]
        if name == "T":
            return tsend.at[key[1], key[2]]
        if name == "R":
            return rrecv.at[key[1], key[2]]
        if name == "N":
            return nsend.at[key[1], key[2]]
        return frecv.at[key[1], key[2]]

    def copy(s, src, dst):
        return pltpu.make_async_remote_copy(
            src_ref=src, dst_ref=dst, send_sem=send_sems.at[s.slot], recv_sem=recv_sems.at[s.sem],
            device_id=peer[s.link], device_id_type=pl.DeviceIdType.MESH,
        )

    def outgoing(s):
        if s.src[0] == "S":
            return copy(s, ssend.at[s.src[1]], srecv.at[s.src[1]])
        if s.dst[0] in parts:
            name, dz, _, part = s.dst
            return copy(s, place(s.src), weight(name, dz, s.src[2], part))
        return copy(s, place(s.src), place(s.dst))

    by_dst = {q.dst: q for q in SENDS if q.only != ()}
    waited = set()

    def arrive(key):
        if key not in by_dst:
            return
        s = by_dst[key]
        if s.sem in waited:
            return
        waited.add(s.sem)
        total = sum({q.dst: q.nbytes for q in SENDS if q.sem == s.sem}.values())
        tall = [k for k in range(1, 9) if total % (8192 * k) == 0 and total // (512 * k) <= ALL_ROWS]
        if total % 8192:
            ref = place(key)
        else:
            ref = xbuf.at[pl.ds(0, tall[0]), pl.ds(0, total // (512 * tall[0])), :]
        copy(s, ref, ref).wait_recv()

    first = {"A": True, "B": True}

    def run(o):
        u = o.unit
        if o.kind == "prep":
            for load in loads[:3]:
                load.wait()
            mine = pl.ds(pl.multiple_of(y * 64, 64), 64)
            g, v, dt = gw[...], uw[...], dw[...]
            wa[0, mine, :] = g[:, :WA].astype(BF16)
            wb[0, mine, pl.ds(0, WA)] = v[:, :WA].astype(BF16)
            mixed = jnp.concatenate([g[:, WA:], v[:, WA:]], axis=1)
            wb[0, mine, pl.ds(WA, 128)] = mixed.astype(BF16)
            for i in range(5):
                dbuf[0, y, pl.ds(i * 64, 64), :] = dt[:, i * 128 : (i + 1) * 128].astype(BF16)
            last = jnp.concatenate([dt[:32, WA:], dt[32:, WA:]], axis=1)
            dbuf[0, y, pl.ds(320, 32), :] = last.astype(BF16)
            pl.semaphore_wait(barrier, 7)
        elif o.kind == "norm":
            for load in loads[3:5]:
                load.wait()
            v = tok[...].astype(F32)
            r = lax.rsqrt(jnp.mean(v * v, axis=-1, keepdims=True) + 1e-06)
            n = (v * r * gain[...]).astype(BF16)
            for k in range(NZ):
                xbuf[(k - zlo + NZ) % NZ, pl.ds(0, ROWS), :] = n[:, k * 256 : (k + 1) * 256]
        elif o.kind in ("mmA", "mmB"):
            n = o.kind[2]
            w, acc = (wa, acca) if n == "A" else (wb, accb)
            start, first[n] = first[n], False

            part = jnp.dot(xbuf[u], w[u], preferred_element_type=F32)
            acc[...] = part if start else acc[...] + part
        elif o.kind == "silu":
            if u == 1:
                for load in loads[5:]:
                    load.wait()
            gs, us = gsc[...].reshape(1, 704), usc[...].reshape(1, 704)
            mixed_scale = jnp.concatenate([gs[:, WA:], us[:, WA:]], axis=1)
            low = lax.broadcasted_iota(jnp.int32, (32, 128), 1) < 64

            @pl.loop(0, 384 // 32)
            def _(i):
                rows = pl.ds(pl.multiple_of(u * 384 + i * 32, 32), 32)
                g = acca[rows, :] * gs[:, :WA]
                v = accb[rows, pl.ds(0, WA)] * us[:, :WA]
                hid[rows, pl.ds(0, WA)] = (silu(g) * v).astype(BF16)
                m = accb[rows, pl.ds(WA, 128)] * mixed_scale
                h = silu(m) * pltpu.roll(m, 64, 1)
                hid[rows, pl.ds(WA, 128)] = jnp.where(low, h, 0.0).astype(BF16)
        elif o.kind in ("dns", "dno"):
            tiles = [dbuf[u, :, pl.ds(i * 64, 64), :].reshape(256, 128) for i in range(5)]
            left = dbuf[u, :, pl.ds(320, 32), :]
            right = pltpu.roll(left.astype(F32).reshape(128, 128), 64, 1).astype(BF16)
            tiles.append(jnp.concatenate([left, right.reshape(4, 32, 128)], axis=1).reshape(256, 128))
            w = jnp.concatenate(tiles, axis=1)
            if o.kind == "dns":
                ssend[u] = nt(hid[pl.ds(384, 384), :], w).astype(BF16)
            else:
                pown[u] = nt(hid[pl.ds(0, 384), :], w)
        elif o.kind == "red1":
            q = pown[u] + srecv[u].astype(F32)
            pown[u] = q
            tsend[u, 0] = q[192:240].astype(BF16)
            tsend[u, 1] = q[240:288].astype(BF16)
        elif o.kind == "red2":
            r0, r1 = rrecv[u, 0].astype(F32), rrecv[u, 1].astype(F32)
            nsend[u, 0, pl.ds(0, 48), :] = (pown[u, pl.ds(288, 48), :] + r0).astype(BF16)
            nsend[u, 0, pl.ds(48, 48), :] = pown[u, pl.ds(336, 48), :].astype(BF16)
            nsend[u, 1, pl.ds(0, 48), :] = pown[u, pl.ds(96, 48), :].astype(BF16)
            nsend[u, 1, pl.ds(48, 48), :] = (pown[u, pl.ds(144, 48), :] + r1).astype(BF16)
        elif o.kind == "fin":
            total = pown[u, pl.ds(0, 96), :] + frecv[u, 0].astype(F32) + frecv[u, 1].astype(F32)
            cols = pl.ds(pl.multiple_of(((zlo + u) % NZ) * 256, 256), 256)
            out[:, cols] = (total * dsc[:, cols]).astype(BF16)

    def active(s):
        return (zg >= s.only[0]) & (zg <= s.only[-1])

    def begin(s):
        if s.only is None:
            outgoing(s).start()
        else:
            pl.when(active(s))(lambda: outgoing(s).start())

    def finish(s):
        if s.only is None:
            outgoing(s).wait_send()
        else:
            pl.when(active(s))(lambda: outgoing(s).wait_send())

    sent = {}
    for o in ORDER:
        if isinstance(o, Send) and o.only == ():
            continue
        for key in o.deps:
            arrive(key)
        if isinstance(o, Send):
            if o.slot in sent:
                finish(sent[o.slot])
            sent[o.slot] = o
            begin(o)
        else:
            run(o)
    for o in sent.values():
        finish(o)


def on_device(
    tokens, norm_gain, gate_weight, up_weight, gate_scale, up_scale, down_weight, down_scale
):
    hbm = pl.BlockSpec(memory_space=pl.ANY)
    vm = pl.BlockSpec(memory_space=pltpu.VMEM)
    return pl.pallas_call(
        kernel,
        out_shape=pltpu.VMEM((ROWS, D), BF16),
        in_specs=[hbm] * 8,
        out_specs=vm,
        scratch_shapes=[
            pltpu.VMEM((ROWS, D), BF16),
            pltpu.VMEM((1, D), F32),
            pltpu.VMEM((64, 704), F32),
            pltpu.VMEM((64, 704), F32),
            pltpu.VMEM((704,), F32),
            pltpu.VMEM((704,), F32),
            pltpu.VMEM((64, 704), F32),
            pltpu.VMEM((1, D), F32),
            pltpu.VMEM((8, ALL_ROWS, 256), BF16),
            pltpu.VMEM((8, 256, WA), BF16),
            pltpu.VMEM((8, 256, WB), BF16),
            pltpu.VMEM((8, 4, 352, 128), BF16),
            pltpu.VMEM((ALL_ROWS, WA), F32),
            pltpu.VMEM((ALL_ROWS, WB), F32),
            pltpu.VMEM((ALL_ROWS, DK), BF16),
            pltpu.VMEM((8, 384, 256), F32),
            pltpu.VMEM((8, 384, 256), BF16),
            pltpu.VMEM((8, 384, 256), BF16),
            pltpu.VMEM((8, 2, 48, 256), BF16),
            pltpu.VMEM((8, 2, 48, 256), BF16),
            pltpu.VMEM((8, 2, 96, 256), BF16),
            pltpu.VMEM((8, 2, 96, 256), BF16),
            pltpu.SemaphoreType.DMA((N_SEND,)),
            pltpu.SemaphoreType.DMA((N_RECV,)),
            pltpu.SemaphoreType.DMA((8,)),
        ],
        compiler_params=pltpu.CompilerParams(
            collective_id=0, has_side_effects=True, vmem_limit_bytes=60 * 1024 * 1024
        ),
    )(
        tokens, norm_gain[None], gate_weight, up_weight, gate_scale, up_scale,
        down_weight.T, down_scale[None],
    )


def solution(mesh):
    placed = (
        P(("rep", "fs", "tp"), None),
        P(),
        P("fs", "tp"),
        P("fs", "tp"),
        P("tp"),
        P("tp"),
        P("tp", "fs"),
        P(),
    )
    return jax.shard_map(
        on_device,
        mesh=mesh,
        in_specs=placed,
        out_specs=P(("rep", "fs", "tp"), None),
        check_vma=False,
    )
```
